32 devices in a mesh: sp: 8 (over z, core), tp: 4 (over y, x).
Axes of the slice: x: 2, y: 2, z: 4, core: 2. Of those that a mesh axis runs over, the one named last changes fastest.
Arguments:
- outer_gate: bfloat16 [2048, 1024], P('sp', 'tp'), may hold values from -6 to 6
- inner_gate: bfloat16 [2048, 1024], P('sp', 'tp'), may hold values from -6 to 6
- values: bfloat16 [2048, 1024], P('sp', 'tp'), may hold values from -6 to 6
- conv_taps: bfloat16 [3, 1024], P(None, 'tp'), may hold values from -3.5 to 3.5
- document: int32 [2048], P('sp'), may hold values from 0 to 3, never falling along the last dimension, each value on 1 to 1024 neighbouring positions
- mix_proj: bfloat16 [1024, 2048], P('tp'), may hold values from -0.1875 to 0.1875
- stream: bfloat16 [2048, 2048], P('sp'), may hold values from -6 to 6
- norm_gain: float32 [2048], replicated, may hold values from 0.1 to 1.9
- routes: int32 [2048, 2], P('sp'), may hold values from 0 to 7, all different within a row; in each aligned block of 256 rows (0 to 255, 256 to 511, ...) at most 96 rows name the same one
- route_weight: float32 [2048, 2], P('sp'), may hold values from 0.25 to 1
- w_gate: bfloat16 [8, 2048, 4096], P('sp', None, 'tp'), may hold values from -0.125 to 0.125
- w_up: bfloat16 [8, 2048, 4096], P('sp', None, 'tp'), may hold values from -0.125 to 0.125
- w_down: bfloat16 [8, 4096, 2048], P('sp', 'tp'), may hold values from -0.09375 to 0.09375
Outputs:
- mixed: bfloat16 [2048, 2048], P('sp', 'tp')
The draws below stay inside these ranges and needn't reach their ends.
Inputs may be any that keep to these rules, and one draw needn't show every extreme that they name: Document numbers never fall along the sequence; each document holds 1 to 1024 consecutive tokens and one holds exactly that many. `routes`: each token names 2 different experts. Among the 256 tokens of one sp index no expert is named by more than 96 tokens, and in some sp index's tokens an expert is named by exactly 96.
All inputs are finite; a program needn't handle non-finite values.
Results may differ from the reference program's by a relative error of at most 0.014.
Values may be sent and summed in bfloat16 or wider, within the bound.
A program may use at most 64 MiB of HBM per device.

```python
import math
import jax
import jax.numpy as jnp
import numpy as np
from jax import lax

D = 2048
DC = 1024
FFE = 4096
TOP = 2
TAPS = 3
T_SP = 256
TOKENS = 2048
EXPERTS = 8
CAP = 96
N_SP = 8
N_TP = 4


def shard_levels(stream_key, shape, shards, smallest, high):
    gain, own = 1.0, jax.random.fold_in(stream_key, 6)
    for dim, shards_of in shards:
        heights = jnp.exp(jax.random.uniform(jax.random.fold_in(own, dim), (shards_of,), jnp.float32, smallest / len(shards), high / len(shards)))
        gain = gain * jnp.repeat(heights, shape[dim] // shards_of).reshape([-1 if axis == dim else 1 for axis in range(len(shape))])
    return gain


def split_up(amount, total, most, slope):
    weights = [(1 << 20) // math.isqrt(standing ** slope) + 1 for standing in range(2, amount + 1)]
    spare, holding = total - most - (amount - 1), [1] * (amount - 1)
    while spare > 0:
        free = [i for i in range(amount - 1) if holding[i] < most]
        pool, remaining = sum([weights[i] for i in free]), spare
        for i in free:
            extra = min(most - holding[i], max(1, remaining * weights[i] // pool), spare)
            holding[i] = holding[i] + extra
            spare = spare - extra
    return np.array([most] + holding)


def ragged(stream_key, number_of, total, most, slope):
    if number_of == 2:
        one = jax.random.randint(stream_key, (), max(1, total - most), min(most, total - 1) + 1)
        return jnp.stack([one, total - one])
    lengths = jnp.asarray(split_up(number_of, total, most, slope), jnp.int32)
    pairs = (number_of - 1) // 2
    source_of, sink = lengths[1:1 + 2 * pairs:2], lengths[2:2 + 2 * pairs:2]
    slack = jnp.minimum(source_of - 1, most - sink)
    moved = jax.random.randint(jax.random.fold_in(stream_key, 1), (pairs,), 0, 1 << 20) % (slack + 1)
    lengths = lengths.at[1:1 + 2 * pairs:2].set(source_of - moved).at[2:2 + 2 * pairs:2].set(sink + moved)
    return lengths[jax.random.permutation(jax.random.fold_in(stream_key, 2), number_of)]


def assign_block(stream_key, own, number, rows, count, top, most, slope):
    ranking = jax.random.permutation(stream_key, count)
    packed, usual = load_shares(count, rows * top, most, slope, True), load_shares(count, rows * top, most, slope, False)
    places = jnp.arange(count)

    def named(lengths, turn):
        used = int((lengths > 0).sum())
        fixed = max(1, used // 4)
        moved = fixed + (places - fixed + turn * (used - fixed)) % max(1, count - fixed)
        return jnp.zeros((count,), jnp.int32).at[ranking[jnp.where(places < fixed, places, moved)]].set(jnp.asarray(lengths, jnp.int32))

    lengths = jnp.where(number % 4 == 0, named(packed, number // 4), named(usual, number - number // 4 - 1))
    mixed = jax.random.permutation(jax.random.fold_in(own, 3), count)
    source_of, taker = mixed[0:count // 2 * 2:2], mixed[1:count // 2 * 2:2]
    margin = jnp.minimum(lengths[source_of] - 1, most - lengths[taker]) // 2
    margin = jnp.where((source_of == ranking[0]) | (taker == ranking[0]) | (lengths[taker] == 0), 0, jnp.maximum(margin, 0))
    moved = jax.random.randint(jax.random.fold_in(own, 4), (count // 2,), 0, 1 << 20) % (margin + 1)
    lengths = lengths.at[source_of].add(-moved).at[taker].add(moved)
    items = jnp.searchsorted(jnp.cumsum(lengths), jnp.arange(rows * top), side="right").astype(jnp.int32)
    listing = items.reshape(top, rows).T
    listing = listing[jax.random.permutation(jax.random.fold_in(own, 1), rows)]
    turn = jax.random.randint(jax.random.fold_in(own, 2), (rows, 1), 0, top)
    return jnp.take_along_axis(listing, (jnp.arange(top)[None, :] + turn) % top, axis=1)


def load_shares(amount, total, bound, lean, full):
    weights = [(1 << 20) // math.isqrt(rank ** lean) + 1 for rank in range(1, amount + 1)]
    largest = bound if full else min(bound, max(-(-total // amount), total * weights[0] // sum(weights)))
    least = 1 if total - largest >= amount - 1 else 0
    counts, rest = [largest] + [least] * (amount - 1), total - largest - least * (amount - 1)
    while rest > 0:
        candidates = [i for i in range(1, amount) if counts[i] < largest] or [i for i in range(1, amount) if counts[i] < bound]
        pool, budget = sum([weights[i] for i in candidates]), rest
        for i in candidates:
            extra = min(bound - counts[i], max(1, budget * weights[i] // pool), rest)
            counts[i] = counts[i] + extra
            rest = rest - extra
    return np.array(counts)


def centred(stream_key, extent, deviation, reach, cuts=(), kind=jnp.bfloat16):
    factor_of = shard_levels(stream_key, extent, cuts, -0.22, 0.18) if cuts else 1.0
    drawn = jax.random.normal(stream_key, extent, jnp.float32) * deviation * factor_of
    return jnp.minimum(jnp.maximum(drawn, -reach), reach).astype(kind)


def setup_inputs(seed: int = 0) -> dict:
    key_list = jax.random.split(jax.random.key(seed), 14)
    outer_gate = centred(key_list[0], (TOKENS, DC), 1.0, 6.0, ((0, 8), (1, 4)))
    inner_gate = centred(key_list[1], (TOKENS, DC), 1.0, 6.0, ((0, 8), (1, 4)))
    values = centred(key_list[2], (TOKENS, DC), 1.0, 6.0, ((0, 8), (1, 4)))
    conv_taps = centred(key_list[3], (TAPS, DC), TAPS ** -0.5, 3.5, ((1, 4),))
    document = jnp.searchsorted(jnp.cumsum(ragged(key_list[4], N_SP // 2, TOKENS, 4 * T_SP, 1)), jnp.arange(TOKENS), side="right").astype(jnp.int32)
    mix_proj = centred(key_list[5], (DC, D), DC ** -0.5, 0.1875, ((0, 4),))
    stream = centred(key_list[6], (TOKENS, D), 1.0, 6.0, ((0, 8),))
    norm_gain = jnp.clip(1.0 + 0.18 * jax.random.normal(key_list[7], (D,), jnp.float32), 0.1, 1.9)
    routes_keys = jax.random.split(jax.random.fold_in(key_list[8], 1), TOKENS // T_SP)
    routes_turns = jax.random.permutation(jax.random.fold_in(key_list[8], 3), TOKENS // T_SP)
    routes = jax.vmap(lambda own, number: assign_block(jax.random.fold_in(key_list[8], 2), own, number, T_SP, EXPERTS, TOP, CAP, 2))(routes_keys, routes_turns).reshape((TOKENS, TOP))
    route_weight = jnp.clip(0.25 + 0.75 * jax.random.uniform(key_list[9], (TOKENS, TOP), jnp.float32) ** shard_levels(key_list[9], (TOKENS, TOP), ((0, 8),), -0.2, 0.2), 0.25, 1.0)
    w_gate = centred(key_list[10], (EXPERTS, D, FFE), D ** -0.5, 0.125, ((0, 8), (2, 4)))
    w_up = centred(key_list[11], (EXPERTS, D, FFE), D ** -0.5, 0.125, ((0, 8), (2, 4)))
    w_down = centred(key_list[12], (EXPERTS, FFE, D), FFE ** -0.5, 0.09375, ((0, 8), (1, 4)))
    return {"outer_gate": outer_gate, "inner_gate": inner_gate, "values": values, "conv_taps": conv_taps, "document": document, "mix_proj": mix_proj, "stream": stream, "norm_gain": norm_gain, "routes": routes, "route_weight": route_weight, "w_gate": w_gate, "w_up": w_up, "w_down": w_down}


def rounded(value):
    held = lax.optimization_barrier(value.astype(jnp.bfloat16))
    return held.astype(jnp.float32)

def reference(outer_gate, inner_gate, values, conv_taps, document, mix_proj, stream, norm_gain, routes, route_weight, w_gate, w_up, w_down):
    length = stream.shape[0]
    product = inner_gate.astype(jnp.float32) * values.astype(jnp.float32)
    kernel = conv_taps.astype(jnp.float32)
    conv = kernel[2] * product
    for back in (1, 2):
        shifted = jnp.pad(product, ((back, 0), (0, 0)))[:length]
        earlier = jnp.pad(document, (back, 0), constant_values=-1)[:length]
        same = (earlier == document)[:, None]
        conv = conv + kernel[2 - back] * jnp.where(same, shifted, 0.0)
    gated = (outer_gate.astype(jnp.float32) * conv).astype(jnp.bfloat16)
    group_width = DC // N_TP
    branch = jnp.zeros((length, D), jnp.float32)
    for group in range(N_TP):
        lower = group * group_width
        partial_value = jnp.dot(gated[:, lower:lower + group_width], mix_proj[lower:lower + group_width], preferred_element_type=jnp.float32)
        branch = branch + rounded(partial_value)
    hidden_state = stream.astype(jnp.float32) + branch
    scale = lax.rsqrt(lax.optimization_barrier(jnp.mean(hidden_state * hidden_state, axis=-1, keepdims=True)) + 1e-06)
    normed = (hidden_state * scale * norm_gain).astype(jnp.bfloat16)
    flat_expert = routes.reshape(-1).astype(jnp.int32)
    count = flat_expert.shape[0]
    flat_token = jnp.arange(count, dtype=jnp.int32) // TOP
    flat_weight = route_weight.reshape(-1)
    order_key = jnp.arange(count, dtype=jnp.int32)
    limit = N_SP * CAP
    hidden_width = FFE // N_TP

    def per_expert(carry, expert):
        keyed = jnp.where(flat_expert == expert, order_key, count)
        chosen = jnp.argsort(keyed, stable=True)[:limit].astype(jnp.int32)
        valid = jnp.take(keyed, chosen) < count
        token_index = jnp.take(flat_token, chosen)
        taken = jnp.take(normed, token_index, axis=0)
        gate = jnp.dot(taken, w_gate[expert], preferred_element_type=jnp.float32)
        upper = jnp.dot(taken, w_up[expert], preferred_element_type=jnp.float32)
        act = (jax.nn.silu(gate) * upper).astype(jnp.bfloat16)
        down = w_down[expert]
        total = jnp.zeros((limit, D), jnp.float32)
        for group in range(N_TP):
            lower = group * hidden_width
            partial_value = jnp.dot(act[:, lower:lower + hidden_width], down[lower:lower + hidden_width], preferred_element_type=jnp.float32)
            total = total + rounded(partial_value)
        expert_out = rounded(total)
        weight = jnp.where(valid, jnp.take(flat_weight, chosen), 0.0)
        carry = carry.at[token_index].add(weight[:, None] * expert_out)
        return (carry, None)
    combined, _ = lax.scan(per_expert, jnp.zeros((length, D), jnp.float32), jnp.arange(EXPERTS, dtype=jnp.int32))
    return (hidden_state + combined).astype(jnp.bfloat16)
```

```python
import functools

import jax
import jax.numpy as jnp
from jax import lax
from jax.experimental import pallas as pl
from jax.experimental.pallas import tpu as pltpu
from jax.sharding import PartitionSpec as P

F32 = jnp.float32
BF16 = jnp.bfloat16
MESH = pl.DeviceIdType.MESH
HEAD = 16
TUNED = (
    (0, 1), (0, 0), (1, 0), (1, 1), (0, 2), (0, 3), (0, 4), (1, 2), (2, 1), (1, 3),
    (0, 5), (1, 4), (3, 1), (4, 1), (6, 1), (0, 6), (1, 5), (2, 2), (0, 7), (3, 2),
    (4, 2), (6, 2), (1, 6), (2, 3), (5, 2), (3, 3), (4, 3), (5, 3), (1, 7), (6, 3),
    (2, 4), (3, 4), (4, 4), (6, 4), (2, 6), (7, 2), (5, 4), (3, 6), (7, 3), (4, 6),
    (6, 6), (5, 6), (2, 5), (8, 2), (3, 5), (4, 5), (7, 4), (5, 5), (6, 5), (8, 3),
    (2, 7), (3, 7), (7, 6), (4, 7), (8, 4), (5, 7), (6, 7), (2, 0), (9, 3), (7, 5),
    (8, 6), (9, 2), (5, 1), (3, 0), (4, 0), (6, 0), (7, 7), (8, 5), (5, 0), (8, 7),
    (7, 1), (9, 4), (7, 0), (9, 6), (9, 5), (8, 1), (9, 1), (9, 7), (8, 0), (9, 0),
)


def general_plan(n_sp):
    plan, near = [], min(2, n_sp)

    def run(k, d, low=0):
        if low <= d < n_sp and (k, d) not in plan:
            plan.append((k, d))

    for k, d in ((0, 0), (0, 1), (1, 0), (0, 2), (1, 1), (0, 3)):
        run(k, d)
    for d in range(n_sp):
        run(2, d)
        run(1, d + 2)
        run(3, d)
        run(0, d + 4)
        run(4, d)
        run(5, d, near)
        run(6, d)
        run(7, d - 2, near)
        run(8, d - 4, near)
        run(9, d - 7, near)
    for d in (n_sp - 2, n_sp - 1):
        run(8, d - 2, near)
        run(7, d, near)
        run(5, n_sp - 1 - d)
    for d in range(near, n_sp):
        run(8, d)
    for d in (1, 0):
        run(7, d)
    for d in range(near, n_sp - 2):
        run(9, d)
    for d in (1, 0):
        run(8, d)
    for d in range(n_sp):
        run(9, d)
    return plan


def xor(value, mask, count):
    out, bit = value, 1
    while bit < count:
        if isinstance(mask, int):
            if mask & bit:
                out = out + bit * (1 - 2 * lax.rem(lax.div(value, bit), 2))
        else:
            ours = lax.rem(lax.div(value, bit), 2)
            other = lax.rem(lax.div(mask, bit), 2)
            out = out + bit * other * (1 - 2 * ours)
        bit *= 2
    return out


def kernel(
    n_sp, n_tp, cap,
    taps_hbm, doc_hbm, routes_hbm, rw_hbm, gain_hbm, outer_hbm, inner_hbm, vals_hbm, mix_hbm, stream_hbm, wg_hbm, wu_hbm, wd_hbm,
    out,
    taps, doc_r, routes_r, rw_r, gain, outer, inner, vals, own, wg, wu, wd, rim_out, rim_in, prod_pad, doc_pad,
    gbuf, mixb, hidden, obuf, xbuf, pbuf, r1, act, ret, back, acc,
    local_sem, rim_s, rim_r, ga_s, ga_r, mx_s, mx_r, z_s, z_r, ag_s, ag_r, rs_s, rs_r, bk_s, bk_r,
):
    s, p = lax.axis_index("sp"), lax.axis_index("tp")
    length, channels = outer.shape
    width = own.shape[1]
    features = mix_hbm.shape[1]
    hidden_units = wg.shape[1]
    x_side = 1
    while x_side * x_side < n_tp:
        x_side *= 2
    square = x_side * x_side == n_tp
    firsts, seconds = range(x_side), range(n_tp // x_side)

    def at(index):
        return pl.multiple_of(index * width, width)

    loads = [
        pltpu.make_async_copy(inner_hbm, inner, local_sem.at[0]),
        pltpu.make_async_copy(vals_hbm, vals, local_sem.at[1]),
        pltpu.make_async_copy(outer_hbm, outer, local_sem.at[2]),
        pltpu.make_async_copy(mix_hbm.at[:, pl.ds(at(p), width)], mixb.at[0], local_sem.at[3]),
        pltpu.make_async_copy(stream_hbm.at[:, pl.ds(at(p), width)], own, local_sem.at[4]),
    ]
    weight_loads = [
        pltpu.make_async_copy(wg_hbm.at[0], wg, local_sem.at[5]),
        pltpu.make_async_copy(wu_hbm.at[0], wu, local_sem.at[6]),
        pltpu.make_async_copy(wd_hbm.at[0], wd, local_sem.at[7]),
    ]
    small_loads = [
        pltpu.make_async_copy(src, dst, local_sem.at[8 + k])
        for k, (src, dst) in enumerate(
            ((routes_hbm, routes_r), (rw_hbm, rw_r), (doc_hbm, doc_r), (taps_hbm, taps), (gain_hbm, gain))
        )
    ]
    for load in small_loads + loads:
        load.start()

    barrier = pltpu.get_barrier_semaphore()
    for d in range(1, n_sp):
        pl.semaphore_signal(barrier, inc=1, device_id={"sp": xor(s, d, n_sp)}, device_id_type=MESH)
    for r in range(1, n_tp):
        pl.semaphore_signal(barrier, inc=1, device_id={"tp": xor(p, r, n_tp)}, device_id_type=MESH)
    sends = []

    def send(src, dst, s_sem, r_sem, **device):
        copy = pltpu.make_async_remote_copy(
            src_ref=src, dst_ref=dst, send_sem=s_sem, recv_sem=r_sem,
            device_id=device, device_id_type=MESH,
        )
        copy.start()
        sends.append(copy)
        return copy

    def arrived(ref, sem):
        pltpu.make_async_copy(ref, ref, sem).wait()

    masks = [m for m in (2, 1) if m < n_sp]
    pieces = 2 ** len(masks)
    piece = channels // pieces

    def piece_rows(mask):
        return pl.ds(pl.multiple_of(lax.rem(xor(s, mask, n_sp), pieces) * piece, piece), piece)

    pl.semaphore_wait(barrier, n_sp - 1 + n_tp - 1)
    for r in range(n_tp - 1, 0, -1):
        peer = xor(p, r, n_tp)
        send(
            mix_hbm.at[piece_rows(0), pl.ds(at(peer), width)], mixb.at[r, piece_rows(0)],
            mx_s.at[0, r], mx_r.at[0, r], tp=peer,
        )

    def pass_on(r, mask, step):
        send(
            mixb.at[r, piece_rows(mask)], mixb.at[r, piece_rows(mask)],
            mx_s.at[step, r], mx_r.at[step, r], sp=xor(s, masks[-1] if step != 1 else masks[0], n_sp),
        )

    for load in small_loads:
        load.wait()
    lines = [routes_r[...].astype(F32), rw_r[...], doc_r[...].astype(F32)]
    table = jnp.concatenate(lines + [jnp.zeros((3, length), F32)], axis=0)
    table = jnp.concatenate([table] * 16, axis=0).T
    chosen = [table[:, 0:1], table[:, 1:2]]
    chosen_weight = [table[:, 2:3], table[:, 3:4]]
    docs = jnp.broadcast_to(table[:, 4:5], (length, channels))
    loads[0].wait()
    loads[1].wait()
    product = inner[...].astype(F32) * vals[...].astype(F32)
    prod_pad[8:, :] = product
    doc_pad[8:, :] = docs
    rim_out[:8, :] = product[length - 8 :]
    rim_out[8:, :] = docs[length - 8 :]
    kernel_taps = taps[...].astype(F32)

    def gated(count):
        conv = kernel_taps[2:3] * product[:count]
        for step in (1, 2):
            same = doc_pad[pl.ds(8 - step, count), :] == docs[:count]
            before = prod_pad[pl.ds(8 - step, count), :]
            conv = conv + kernel_taps[2 - step : 3 - step] * jnp.where(same, before, 0.0)
        return (outer[:count, :].astype(F32) * conv).astype(BF16)

    has_next = s < n_sp - 1
    rim = pltpu.make_async_remote_copy(
        src_ref=rim_out, dst_ref=rim_in, send_sem=rim_s, recv_sem=rim_r,
        device_id={"sp": lax.rem(s + 1, n_sp)}, device_id_type=MESH,
    )

    @pl.when(has_next)
    def _():
        rim.start()

    prod_pad[:8, :] = jnp.zeros((8, channels), F32)
    doc_pad[:8, :] = jnp.full((8, channels), -1.0, F32)
    loads[2].wait()
    gbuf[0] = gated(length)

    @pl.when(s > 0)
    def _():
        rim.wait_recv()
        prod_pad[:8, :] = rim_in[:8, :]
        doc_pad[:8, :] = rim_in[8:, :]
        gbuf[0, :HEAD] = gated(HEAD)

    for r in range(n_tp - 1, 0, -1):
        send(gbuf.at[0], gbuf.at[r], ga_s.at[r], ga_r.at[r], tp=xor(p, r, n_tp))
    for load in weight_loads:
        load.start()

    row = lax.broadcasted_iota(jnp.int32, (length, length), 0)
    col = lax.broadcasted_iota(jnp.int32, (length, length), 1)
    expert_r = lax.broadcasted_iota(jnp.int32, (max(n_sp, 16), length), 0)
    in_r = ((routes_r[0:1, :] == expert_r) | (routes_r[1:2, :] == expert_r)).astype(F32)
    rank_r = jnp.dot(in_r.astype(BF16), (row < col).astype(F32).astype(BF16), preferred_element_type=F32)
    expert_c = lax.broadcasted_iota(jnp.int32, (length, 128), 1).astype(F32)
    in_c = ((chosen[0] == expert_c) | (chosen[1] == expert_c)).astype(F32)
    rank_c = jnp.dot((row > col).astype(F32).astype(BF16), in_c.astype(BF16), preferred_element_type=F32)
    rank_r = jnp.where(in_r > 0, rank_r, -1.0)
    rank_c = jnp.where(in_c > 0, rank_c, -1.0)

    for r in range(n_tp - 1, 0, -1):
        arrived(mixb.at[r, piece_rows(0)], mx_r.at[0, r])
        if len(masks) == 2:
            pass_on(r, 0, 1)
        if masks:
            pass_on(r, 0, 2)
    loads[3].wait()
    loads[4].wait()
    total = own[...].astype(F32) + jnp.dot(gbuf[0], mixb[0], preferred_element_type=F32)
    if len(masks) == 2:
        for r in range(n_tp - 1, 0, -1):
            arrived(mixb.at[r, piece_rows(2)], mx_r.at[1, r])
            pass_on(r, 2, 3)
    for r in range(n_tp - 1, 0, -1):
        if masks:
            arrived(mixb.at[r, piece_rows(1)], mx_r.at[2, r])
        if len(masks) == 2:
            arrived(mixb.at[r, piece_rows(3)], mx_r.at[3, r])
        arrived(gbuf.at[r], ga_r.at[r])
        total = total + jnp.dot(gbuf[r], mixb[r], preferred_element_type=F32)
    hidden[...] = total
    scaled = (total * gain[:, pl.ds(at(p), width)]).astype(BF16)

    slot_r = lax.broadcasted_iota(jnp.int32, (cap, length), 0).astype(F32)
    turn = [0, 1, 2, 3, 4, 6, 5, 7] + list(range(8, n_sp))
    for d in range(n_sp):
        e = xor(s, turn[d], n_sp)
        line = jnp.sum(jnp.where(expert_r == e, rank_r, 0.0), axis=0, keepdims=True)
        pick = (line == slot_r).astype(F32).astype(BF16)
        rows = jnp.dot(pick, scaled, preferred_element_type=F32).astype(BF16)
        if d == 0:
            xbuf[0, 0] = rows
        else:
            obuf[d] = rows
            send(obuf.at[d], xbuf.at[0, d], z_s.at[d], z_r.at[d], sp=e)

    def axes(d):
        side = lax.rem(s + d, 2) * (x_side - 1) if square else 0
        return 1 + side, x_side - side

    def gather_first(d):
        u, _ = axes(d)
        if d:
            arrived(xbuf.at[0, d], z_r.at[d])
        for k in firsts[1:]:
            f = k * u
            send(xbuf.at[0, d], xbuf.at[f, d], ag_s.at[d, f], ag_r.at[d, f], tp=xor(p, f, n_tp))

    def gather_second(d):
        u, v = axes(d)
        for k in firsts:
            f = k * u
            if k:
                arrived(xbuf.at[f, d], ag_r.at[d, f])
            for l in seconds[1:]:
                g = l * v
                send(
                    xbuf.at[f, d], xbuf.at[f + g, d], ag_s.at[d, f + g], ag_r.at[d, f + g],
                    tp=xor(p, g, n_tp),
                )

    tile = min(256, hidden_units)
    tiles = hidden_units // tile

    scales = {}

    def up_part(d, low, high):
        def up_tile(j, _):
            lanes = pl.ds(pl.multiple_of(j * tile, tile), tile)
            gate = jnp.zeros((cap, tile), F32)
            upper = jnp.zeros((cap, tile), F32)
            for r in range(n_tp):
                lhs = xbuf[r, d]
                deep = pl.ds(at(xor(p, r, n_tp)), width)
                gate = gate + jnp.dot(lhs, wg[deep, lanes], preferred_element_type=F32)
                upper = upper + jnp.dot(lhs, wu[deep, lanes], preferred_element_type=F32)
            gate, upper = gate * scales[d], upper * scales[d]
            act[:, lanes] = (gate / (1.0 + jnp.exp(-gate)) * upper).astype(BF16)
            return 0

        lax.fori_loop(low, high, up_tile, 0)

    def up_first(d):
        u, v = axes(d)
        for k in firsts:
            for l in seconds[1:]:
                arrived(xbuf.at[k * u + l * v, d], ag_r.at[d, k * u + l * v])
        power = jnp.zeros((cap, 1), F32)
        for r in range(n_tp):
            inverse = 1.0 / gain[:, pl.ds(at(xor(p, r, n_tp)), width)]
            plain = xbuf[r, d].astype(F32) * inverse
            power = power + jnp.sum(plain * plain, axis=1, keepdims=True)
        scales[d] = lax.rsqrt(power / features + 1e-06)
        up_part(d, 0, tiles // 2)

    def up_second(d):
        up_part(d, tiles // 2, tiles)

    def down_part(d, low, high):
        u, v = axes(d)
        for k in range(low, high):
            for l in seconds[::-1]:
                r = k * u + l * v
                lanes = pl.ds(at(xor(p, r, n_tp)), width)
                pbuf[r, d] = jnp.dot(act[...], wd[:, lanes], preferred_element_type=F32).astype(BF16)

    def down_first(d):
        down_part(d, 1, len(firsts))

    def down_second(d):
        down_part(d, 0, 1)

    def scatter_first(d):
        u, v = axes(d)
        for k in firsts[:0:-1]:
            for l in seconds[::-1]:
                r = k * u + l * v
                send(pbuf.at[r, d], r1.at[r, d], rs_s.at[d, r], rs_r.at[d, r], tp=xor(p, k * u, n_tp))

    def scatter_second(d):
        u, v = axes(d)
        for l in seconds[1:]:
            g = l * v
            part = pbuf[g, d].astype(F32)
            for k in firsts[1:]:
                arrived(r1.at[k * u + g, d], rs_r.at[d, k * u + g])
                part = part + r1[k * u + g, d].astype(F32)
            pbuf[g, d] = part.astype(BF16)
            send(pbuf.at[g, d], r1.at[g, d], rs_s.at[d, g], rs_r.at[d, g], tp=xor(p, g, n_tp))

    def give_back(d):
        u, v = axes(d)
        part = pbuf[0, d].astype(F32)
        for k in [k * u for k in firsts[1:]] + [l * v for l in seconds[1:]]:
            arrived(r1.at[k, d], rs_r.at[d, k])
            part = part + r1[k, d].astype(F32)
        if d == 0:
            back[0] = part.astype(BF16)
        else:
            ret[d] = part.astype(BF16)
            send(ret.at[d], back.at[d], bk_s.at[d], bk_r.at[d], sp=xor(s, turn[d], n_sp))

    slot_c = lax.broadcasted_iota(jnp.int32, (length, cap), 1).astype(F32)
    acc[...] = hidden[...]

    def combine(d):
        e = xor(s, turn[d], n_sp)
        if d:
            arrived(back.at[d], bk_r.at[d])
        line = jnp.sum(jnp.where(expert_c == e.astype(F32), rank_c, 0.0), axis=1, keepdims=True)
        pick = (line == slot_c).astype(F32).astype(BF16)
        fetched = jnp.dot(pick, back[d], preferred_element_type=F32)
        weight = sum(jnp.where(c == e.astype(F32), w, 0.0) for c, w in zip(chosen, chosen_weight))
        acc[...] = acc[...] + fetched * weight

    stages = (
        gather_first, gather_second, up_first, up_second, down_first,
        scatter_first, down_second, scatter_second, give_back, combine,
    )
    plan = TUNED if len(TUNED) == len(stages) * n_sp else general_plan(n_sp)
    weights_here = False
    for k, d in plan:
        stage = stages[k]
        if stage is up_first and not weights_here:
            weights_here = True
            for load in weight_loads:
                load.wait()
        stage(d)
    out[...] = acc[...].astype(out.dtype)
    for copy in sends:
        copy.wait_send()

    @pl.when(has_next)
    def _():
        rim.wait_send()


def body(
    outer_gate, inner_gate, values, conv_taps, document, mix_proj, stream, norm_gain,
    routes, route_weight, w_gate, w_up, w_down,
):
    length, features = stream.shape
    channels = outer_gate.shape[1]
    n_sp, n_tp = lax.axis_size("sp"), lax.axis_size("tp")
    width = features // n_tp
    units = w_gate.shape[2]
    cap = -(-(3 * length // n_sp) // 16) * 16
    vmem, hbm = pl.BlockSpec(memory_space=pltpu.VMEM), pl.BlockSpec(memory_space=pltpu.HBM)
    block = (n_sp, cap, width)
    dma = pltpu.SemaphoreType.DMA
    return pl.pallas_call(
        functools.partial(kernel, n_sp, n_tp, cap),
        out_shape=pltpu.VMEM((length, width), BF16),
        in_specs=[hbm] * 13,
        out_specs=vmem,
        scratch_shapes=[
            pltpu.VMEM(conv_taps.shape, BF16),
            pltpu.VMEM((1, length), jnp.int32),
            pltpu.VMEM((2, length), jnp.int32),
            pltpu.VMEM((2, length), F32),
            pltpu.VMEM((1, features), F32),
            pltpu.VMEM((length, channels), BF16),
            pltpu.VMEM((length, channels), BF16),
            pltpu.VMEM((length, channels), BF16),
            pltpu.VMEM((length, width), BF16),
            pltpu.VMEM((features, units), BF16),
            pltpu.VMEM((features, units), BF16),
            pltpu.VMEM((units, features), BF16),
            pltpu.VMEM((16, channels), F32),
            pltpu.VMEM((16, channels), F32),
            pltpu.VMEM((length + 8, channels), F32),
            pltpu.VMEM((length + 8, channels), F32),
            pltpu.VMEM((n_tp, length, channels), BF16),
            pltpu.VMEM((n_tp, channels, width), BF16),
            pltpu.VMEM((length, width), F32),
            pltpu.VMEM(block, BF16),
            pltpu.VMEM((n_tp,) + block, BF16),
            pltpu.VMEM((n_tp,) + block, BF16),
            pltpu.VMEM((n_tp,) + block, BF16),
            pltpu.VMEM((cap, units), BF16),
            pltpu.VMEM(block, BF16),
            pltpu.VMEM(block, BF16),
            pltpu.VMEM((length, width), F32),
            dma((13,)), dma, dma, dma((n_tp,)), dma((n_tp,)), dma((4, n_tp)), dma((4, n_tp)), dma((n_sp,)), dma((n_sp,)),
            dma((n_sp, n_tp)), dma((n_sp, n_tp)), dma((n_sp, n_tp)), dma((n_sp, n_tp)),
            dma((n_sp,)), dma((n_sp,)),
        ],
        compiler_params=pltpu.CompilerParams(
            collective_id=0, has_side_effects=True, vmem_limit_bytes=40 << 20
        ),
    )(*[pltpu.with_memory_space_constraint(x, pltpu.HBM) for x in (
        conv_taps, document.reshape(1, -1), routes.T, route_weight.T, norm_gain.reshape(1, -1),
        outer_gate, inner_gate, values, mix_proj, stream, w_gate, w_up, w_down,
    )])


def solution(mesh):
    return jax.shard_map(
        body,
        mesh=mesh,
        in_specs=(
            P("sp", "tp"),
            P("sp", "tp"),
            P("sp", "tp"),
            P(None, "tp"),
            P("sp"),
            P("tp", None),
            P("sp", None),
            P(),
            P("sp", None),
            P("sp", None),
            P("sp", None, "tp"),
            P("sp", None, "tp"),
            P("sp", "tp", None),
        ),
        out_specs=P("sp", "tp"),
        check_vma=False,
    )
```

```python
import functools

import jax
import jax.numpy as jnp
from jax import lax
from jax.experimental import pallas as pl
from jax.experimental.pallas import tpu as pltpu
from jax.sharding import PartitionSpec as P

F32 = jnp.float32
BF16 = jnp.bfloat16
MESH = pl.DeviceIdType.MESH
HEAD = 16
TUNED = (
    (0, 0), (1, 0), (0, 1), (0, 2), (1, 1), (0, 4), (1, 2), (0, 3),
    (0, 5), (1, 4), (2, 0), (0, 6), (1, 5), (0, 7), (3, 0), (4, 0),
    (6, 0), (1, 6), (1, 3), (2, 2), (1, 7), (3, 2), (4, 2), (5, 5),
    (6, 2), (5, 4), (5, 0), (2, 3), (7, 5), (3, 3), (4, 3), (6, 3),
    (5, 6), (7, 4), (2, 1), (5, 7), (8, 5), (3, 1), (4, 1), (7, 6),
    (5, 3), (8, 4), (5, 2), (9, 5), (8, 6), (7, 7), (6, 1), (7, 3),
    (5, 1), (9, 4), (8, 7), (7, 2), (8, 3), (7, 1), (7, 0), (8, 2),
    (9, 3), (8, 1), (9, 6), (8, 0), (9, 0), (9, 7), (9, 1), (9, 2),
)


def general_plan(n_sp, group):
    plan, near = [], min(2, n_sp)

    def run(k, d, low=0):
        if low <= d < n_sp and (k, d) not in plan:
            plan.append((k, d))

    for k, d in ((0, 0), (0, 1), (1, 0), (1, 1), (0, 2), (0, 3), (1, 2)):
        run(k, d)
    for j in range(n_sp // group):
        first = j * group
        ahead, behind = range(first + 3, first + 3 + group), range(first - group, first)
        plan.append((2, j))
        for d in ahead:
            run(0, d + 1)
        plan.append((3, j))
        for d in ahead:
            run(1, d)
        plan.append((4, j))
        for d in range(first, first + group):
            run(5, d, near)
        plan.append((6, j))
        for d in behind:
            run(7, d, near)
        for d in behind:
            run(8, d - group, near)
        for d in behind:
            run(9, d - 3 * group, near)
    for d in range(near, n_sp):
        run(8, d - group, near)
        run(7, d, near)
        run(5, n_sp - 1 - d)
    for d in (1, 0):
        run(5, d)
    for d in range(near, n_sp):
        run(8, d)
    for d in (1, 0):
        run(7, d)
    for d in range(near, n_sp - 2):
        run(9, d)
    for d in (1, 0):
        run(8, d)
    for d in range(n_sp):
        run(9, d)
    return plan


def xor(value, mask, count):
    out, bit = value, 1
    while bit < count:
        if isinstance(mask, int):
            if mask & bit:
                out = out + bit * (1 - 2 * lax.rem(lax.div(value, bit), 2))
        else:
            ours = lax.rem(lax.div(value, bit), 2)
            other = lax.rem(lax.div(mask, bit), 2)
            out = out + bit * other * (1 - 2 * ours)
        bit *= 2
    return out


def kernel(
    n_sp, n_tp, cap,
    taps_hbm, doc_hbm, routes_hbm, rw_hbm, gain_hbm, outer_hbm, inner_hbm, vals_hbm, mix_hbm, stream_hbm, wg_hbm, wu_hbm, wd_hbm,
    out,
    taps, doc_r, routes_r, rw_r, gain, outer, inner, vals, own, wg, wu, wd, rim_out, rim_in, prod_pad, doc_pad,
    gbuf, mixb, hidden, obuf, xbuf, pbuf, r1, act, ret, back, acc,
    local_sem, rim_s, rim_r, ga_s, ga_r, mx_s, mx_r, z_s, z_r, ag_s, ag_r, rs_s, rs_r, bk_s, bk_r,
):
    s, p = lax.axis_index("sp"), lax.axis_index("tp")
    length, channels = outer.shape
    width = own.shape[1]
    features = mix_hbm.shape[1]
    hidden_units = wg.shape[1]
    x_side = 1
    while x_side * x_side < n_tp:
        x_side *= 2
    square = x_side * x_side == n_tp
    group = 2 if n_sp % 2 == 0 else 1
    firsts, seconds = range(x_side), range(n_tp // x_side)

    def at(index):
        return pl.multiple_of(index * width, width)

    masks = [m for m in (2, 1) if m < n_sp]
    pieces = 2 ** len(masks)
    piece = channels // pieces

    def piece_rows(mask):
        return pl.ds(pl.multiple_of(lax.rem(xor(s, mask, n_sp), pieces) * piece, piece), piece)

    loads = [
        pltpu.make_async_copy(inner_hbm, inner, local_sem.at[0]),
        pltpu.make_async_copy(vals_hbm, vals, local_sem.at[1]),
        pltpu.make_async_copy(outer_hbm, outer, local_sem.at[2]),
        pltpu.make_async_copy(mix_hbm.at[:, pl.ds(at(p), width)], mixb.at[0], local_sem.at[3]),
        pltpu.make_async_copy(stream_hbm.at[:, pl.ds(at(p), width)], own, local_sem.at[4]),
    ]
    weight_loads = [
        pltpu.make_async_copy(wg_hbm.at[0], wg, local_sem.at[5]),
        pltpu.make_async_copy(wu_hbm.at[0], wu, local_sem.at[6]),
        pltpu.make_async_copy(wd_hbm.at[0], wd, local_sem.at[7]),
    ]
    small_loads = [
        pltpu.make_async_copy(src, dst, local_sem.at[8 + k])
        for k, (src, dst) in enumerate(
            ((routes_hbm, routes_r), (rw_hbm, rw_r), (doc_hbm, doc_r), (taps_hbm, taps), (gain_hbm, gain))
        )
    ]
    for load in small_loads + loads:
        load.start()

    barrier = pltpu.get_barrier_semaphore()
    for d in range(1, n_sp):
        pl.semaphore_signal(barrier, inc=1, device_id={"sp": xor(s, d, n_sp)}, device_id_type=MESH)
    for r in range(1, n_tp):
        pl.semaphore_signal(barrier, inc=1, device_id={"tp": xor(p, r, n_tp)}, device_id_type=MESH)
    def send(src, dst, s_sem, r_sem, **device):
        pltpu.make_async_remote_copy(
            src_ref=src, dst_ref=dst, send_sem=s_sem, recv_sem=r_sem,
            device_id=device, device_id_type=MESH,
        ).start()

    def arrived(ref, sem):
        pltpu.make_async_copy(ref, ref, sem).wait()

    pl.semaphore_wait(barrier, n_sp - 1 + n_tp - 1)
    for r in range(n_tp - 1, 0, -1):
        peer = xor(p, r, n_tp)
        send(
            mix_hbm.at[piece_rows(0), pl.ds(at(peer), width)], mixb.at[r, piece_rows(0)],
            mx_s, mx_r.at[0, r], tp=peer,
        )

    def pass_on(r, mask, step):
        send(
            mixb.at[r, piece_rows(mask)], mixb.at[r, piece_rows(mask)],
            mx_s, mx_r.at[step, r], sp=xor(s, masks[-1] if step != 1 else masks[0], n_sp),
        )

    for load in small_loads:
        load.wait()
    lines = [routes_r[...].astype(F32), rw_r[...], doc_r[...].astype(F32)]
    table = jnp.concatenate(lines + [jnp.zeros((3, length), F32)], axis=0)
    table = jnp.concatenate([table] * 16, axis=0).T
    chosen = [table[:, 0:1], table[:, 1:2]]
    chosen_weight = [table[:, 2:3], table[:, 3:4]]
    docs = jnp.broadcast_to(table[:, 4:5], (length, channels))
    loads[0].wait()
    loads[1].wait()
    product = inner[...].astype(F32) * vals[...].astype(F32)
    prod_pad[8:, :] = product
    doc_pad[8:, :] = docs
    rim_out[:8, :] = product[length - 8 :]
    rim_out[8:, :] = docs[length - 8 :]
    kernel_taps = taps[...].astype(F32)

    def gated(count):
        conv = kernel_taps[2:3] * product[:count]
        for step in (1, 2):
            same = doc_pad[pl.ds(8 - step, count), :] == docs[:count]
            before = prod_pad[pl.ds(8 - step, count), :]
            conv = conv + kernel_taps[2 - step : 3 - step] * jnp.where(same, before, 0.0)
        return (outer[:count, :].astype(F32) * conv).astype(BF16)

    has_next = s < n_sp - 1
    rim = pltpu.make_async_remote_copy(
        src_ref=rim_out, dst_ref=rim_in, send_sem=rim_s, recv_sem=rim_r,
        device_id={"sp": lax.rem(s + 1, n_sp)}, device_id_type=MESH,
    )

    @pl.when(has_next)
    def _():
        rim.start()

    prod_pad[:8, :] = jnp.zeros((8, channels), F32)
    doc_pad[:8, :] = jnp.full((8, channels), -1.0, F32)
    loads[2].wait()
    gbuf[0] = gated(length)

    @pl.when(s > 0)
    def _():
        rim.wait_recv()
        prod_pad[:8, :] = rim_in[:8, :]
        doc_pad[:8, :] = rim_in[8:, :]
        gbuf[0, :HEAD] = gated(HEAD)

    for r in range(n_tp - 1, 0, -1):
        send(gbuf.at[0], gbuf.at[r], ga_s, ga_r.at[r], tp=xor(p, r, n_tp))
    for load in weight_loads:
        load.start()

    row = lax.broadcasted_iota(jnp.int32, (length, length), 0)
    col = lax.broadcasted_iota(jnp.int32, (length, length), 1)
    expert_r = lax.broadcasted_iota(jnp.int32, (max(n_sp, 16), length), 0)
    in_r = ((routes_r[0:1, :] == expert_r) | (routes_r[1:2, :] == expert_r)).astype(F32)
    rank_r = jnp.dot(in_r.astype(BF16), (row < col).astype(F32).astype(BF16), preferred_element_type=F32)
    expert_c = lax.broadcasted_iota(jnp.int32, (length, 128), 1).astype(F32)
    in_c = ((chosen[0] == expert_c) | (chosen[1] == expert_c)).astype(F32)
    rank_c = jnp.dot((row > col).astype(F32).astype(BF16), in_c.astype(BF16), preferred_element_type=F32)
    rank_r = jnp.where(in_r > 0, rank_r, -1.0)
    rank_c = jnp.where(in_c > 0, rank_c, -1.0)

    slot_r = lax.broadcasted_iota(jnp.int32, (cap, length), 0).astype(F32)
    turn = [0, 1, 2, 3, 4, 6, 5, 7] + list(range(8, n_sp))
    picks = []
    for d in range(n_sp):
        line = jnp.sum(jnp.where(expert_r == xor(s, turn[d], n_sp), rank_r, 0.0), axis=0, keepdims=True)
        picks.append((line == slot_r).astype(F32).astype(BF16))

    for r in range(n_tp - 1, 0, -1):
        arrived(mixb.at[r, piece_rows(0)], mx_r.at[0, r])
        if len(masks) == 2:
            pass_on(r, 0, 1)
        if masks:
            pass_on(r, 0, 2)
    loads[3].wait()
    loads[4].wait()
    total = own[...].astype(F32) + jnp.dot(gbuf[0], mixb[0], preferred_element_type=F32)
    if len(masks) == 2:
        for r in range(n_tp - 1, 0, -1):
            arrived(mixb.at[r, piece_rows(2)], mx_r.at[1, r])
            pass_on(r, 2, 3)
    for r in range(n_tp - 1, 0, -1):
        if masks:
            arrived(mixb.at[r, piece_rows(1)], mx_r.at[2, r])
        if len(masks) == 2:
            arrived(mixb.at[r, piece_rows(3)], mx_r.at[3, r])
        arrived(gbuf.at[r], ga_r.at[r])
        total = total + jnp.dot(gbuf[r], mixb[r], preferred_element_type=F32)
    hidden[...] = total
    scaled = (total * gain[:, pl.ds(at(p), width)]).astype(BF16)

    for d in range(n_sp):
        rows = jnp.dot(picks[d], scaled, preferred_element_type=F32).astype(BF16)
        if d == 0:
            xbuf[0, 0] = rows
        else:
            obuf[d] = rows
            send(obuf.at[d], xbuf.at[0, d], z_s, z_r.at[d], sp=xor(s, turn[d], n_sp))

    def axes(d):
        side = lax.rem(s + d // group, 2) * (x_side - 1) if square else 0
        return 1 + side, x_side - side

    def gather_first(d):
        u, _ = axes(d)
        if d:
            arrived(xbuf.at[0, d], z_r.at[d])
        for k in firsts[1:]:
            f = k * u
            send(xbuf.at[0, d], xbuf.at[f, d], ag_s, ag_r.at[d, f], tp=xor(p, f, n_tp))

    def gather_second(d):
        u, v = axes(d)
        for k in firsts:
            f = k * u
            if k:
                arrived(xbuf.at[f, d], ag_r.at[d, f])
            for l in seconds[1:]:
                g = l * v
                send(
                    xbuf.at[f, d], xbuf.at[f + g, d], ag_s, ag_r.at[d, f + g],
                    tp=xor(p, g, n_tp),
                )

    tile = min(256, hidden_units)
    tiles = hidden_units // tile

    scales = {}

    def members(j):
        return slice(j * group, (j + 1) * group)

    def up_part(j, low, high):
        def up_tile(i, _):
            lanes = pl.ds(pl.multiple_of(i * tile, tile), tile)
            gate = jnp.zeros((group * cap, tile), F32)
            upper = jnp.zeros((group * cap, tile), F32)
            for r in range(n_tp):
                lhs = xbuf[r, members(j)].reshape(group * cap, width)
                deep = pl.ds(at(xor(p, r, n_tp)), width)
                gate = gate + jnp.dot(lhs, wg[deep, lanes], preferred_element_type=F32)
                upper = upper + jnp.dot(lhs, wu[deep, lanes], preferred_element_type=F32)
            gate, upper = gate * scales[j], upper * scales[j]
            act[:, lanes] = (gate / (1.0 + jnp.exp(-gate)) * upper).astype(BF16)
            return 0

        lax.fori_loop(low, high, up_tile, 0)

    def up_first(j):
        if not scales:
            for load in weight_loads:
                load.wait()
        u, v = axes(j * group)
        for d in range(j * group, (j + 1) * group):
            for k in firsts:
                for l in seconds[1:]:
                    arrived(xbuf.at[k * u + l * v, d], ag_r.at[d, k * u + l * v])
        power = jnp.zeros((group * cap, 1), F32)
        for r in range(n_tp):
            inverse = 1.0 / gain[:, pl.ds(at(xor(p, r, n_tp)), width)]
            plain = xbuf[r, members(j)].reshape(group * cap, width).astype(F32) * inverse
            power = power + jnp.sum(plain * plain, axis=1, keepdims=True)
        scales[j] = lax.rsqrt(power / features + 1e-06)
        up_part(j, 0, tiles // 2)

    def up_second(j):
        up_part(j, tiles // 2, tiles)

    def down_part(j, low, high):
        u, v = axes(j * group)
        for k in range(low, high):
            for l in seconds[::-1]:
                r = k * u + l * v
                lanes = pl.ds(at(xor(p, r, n_tp)), width)
                part = jnp.dot(act[...], wd[:, lanes], preferred_element_type=F32).astype(BF16)
                pbuf[r, members(j)] = part.reshape(group, cap, width)

    def down_first(j):
        down_part(j, 1, len(firsts))

    def down_second(j):
        down_part(j, 0, 1)

    def scatter_first(d):
        u, v = axes(d)
        for k in firsts[:0:-1]:
            for l in seconds[::-1]:
                r = k * u + l * v
                send(pbuf.at[r, d], r1.at[r, d], rs_s, rs_r.at[d, r], tp=xor(p, k * u, n_tp))

    def scatter_second(d):
        u, v = axes(d)
        for l in seconds[1:]:
            g = l * v
            part = pbuf[g, d].astype(F32)
            for k in firsts[1:]:
                arrived(r1.at[k * u + g, d], rs_r.at[d, k * u + g])
                part = part + r1[k * u + g, d].astype(F32)
            pbuf[g, d] = part.astype(BF16)
            send(pbuf.at[g, d], r1.at[g, d], rs_s, rs_r.at[d, g], tp=xor(p, g, n_tp))

    def give_back(d):
        u, v = axes(d)
        part = pbuf[0, d].astype(F32)
        for k in [k * u for k in firsts[1:]] + [l * v for l in seconds[1:]]:
            arrived(r1.at[k, d], rs_r.at[d, k])
            part = part + r1[k, d].astype(F32)
        if d == 0:
            back[0] = part.astype(BF16)
        else:
            ret[d] = part.astype(BF16)
            send(ret.at[d], back.at[d], bk_s, bk_r.at[d], sp=xor(s, turn[d], n_sp))

    slot_c = lax.broadcasted_iota(jnp.int32, (length, cap), 1).astype(F32)
    acc[...] = hidden[...]

    def combine(d):
        e = xor(s, turn[d], n_sp)
        if d:
            arrived(back.at[d], bk_r.at[d])
        line = jnp.sum(jnp.where(expert_c == e.astype(F32), rank_c, 0.0), axis=1, keepdims=True)
        pick = (line == slot_c).astype(F32).astype(BF16)
        fetched = jnp.dot(pick, back[d], preferred_element_type=F32)
        weight = sum(jnp.where(c == e.astype(F32), w, 0.0) for c, w in zip(chosen, chosen_weight))
        acc[...] = acc[...] + fetched * weight

    stages = (
        gather_first, gather_second, up_first, up_second, down_first,
        scatter_first, down_second, scatter_second, give_back, combine,
    )
    plan = general_plan(n_sp, group)
    plan = TUNED if len(TUNED) == len(plan) else plan
    for k, d in plan[:-1]:
        stages[k](d)
    arrived(xbuf.at[0, pl.ds(1, n_sp - 1)], z_s)
    arrived(back.at[pl.ds(1, n_sp - 1)], bk_s)
    arrived(gbuf.at[pl.ds(1, n_tp - 1)], ga_s)
    arrived(xbuf.at[pl.ds(1, n_tp - 1)], ag_s)
    arrived(r1.at[pl.ds(1, n_tp - 1)], rs_s)
    arrived(mixb.at[pl.ds(1, n_tp - 1)], mx_s)
    stages[plan[-1][0]](plan[-1][1])
    out[...] = acc[...].astype(out.dtype)
    @pl.when(has_next)
    def _():
        rim.wait_send()


def body(
    outer_gate, inner_gate, values, conv_taps, document, mix_proj, stream, norm_gain,
    routes, route_weight, w_gate, w_up, w_down,
):
    length, features = stream.shape
    channels = outer_gate.shape[1]
    n_sp, n_tp = lax.axis_size("sp"), lax.axis_size("tp")
    width = features // n_tp
    units = w_gate.shape[2]
    cap = -(-(3 * length // n_sp) // 16) * 16
    vmem, hbm = pl.BlockSpec(memory_space=pltpu.VMEM), pl.BlockSpec(memory_space=pltpu.HBM)
    block = (n_sp, cap, width)
    dma = pltpu.SemaphoreType.DMA
    return pl.pallas_call(
        functools.partial(kernel, n_sp, n_tp, cap),
        out_shape=pltpu.VMEM((length, width), BF16),
        in_specs=[hbm] * 13,
        out_specs=vmem,
        scratch_shapes=[
            pltpu.VMEM(conv_taps.shape, BF16),
            pltpu.VMEM((1, length), jnp.int32),
            pltpu.VMEM((2, length), jnp.int32),
            pltpu.VMEM((2, length), F32),
            pltpu.VMEM((1, features), F32),
            pltpu.VMEM((length, channels), BF16),
            pltpu.VMEM((length, channels), BF16),
            pltpu.VMEM((length, channels), BF16),
            pltpu.VMEM((length, width), BF16),
            pltpu.VMEM((features, units), BF16),
            pltpu.VMEM((features, units), BF16),
            pltpu.VMEM((units, features), BF16),
            pltpu.VMEM((16, channels), F32),
            pltpu.VMEM((16, channels), F32),
            pltpu.VMEM((length + 8, channels), F32),
            pltpu.VMEM((length + 8, channels), F32),
            pltpu.VMEM((n_tp, length, channels), BF16),
            pltpu.VMEM((n_tp, channels, width), BF16),
            pltpu.VMEM((length, width), F32),
            pltpu.VMEM(block, BF16),
            pltpu.VMEM((n_tp,) + block, BF16),
            pltpu.VMEM((n_tp,) + block, BF16),
            pltpu.VMEM((n_tp,) + block, BF16),
            pltpu.VMEM(((2 if n_sp % 2 == 0 else 1) * cap, units), BF16),
            pltpu.VMEM(block, BF16),
            pltpu.VMEM(block, BF16),
            pltpu.VMEM((length, width), F32),
            dma((13,)), dma, dma, dma, dma((n_tp,)), dma, dma((4, n_tp)), dma, dma((n_sp,)),
            dma, dma((n_sp, n_tp)), dma, dma((n_sp, n_tp)),
            dma, dma((n_sp,)),
        ],
        compiler_params=pltpu.CompilerParams(
            collective_id=0, has_side_effects=True, vmem_limit_bytes=40 << 20
        ),
    )(*[pltpu.with_memory_space_constraint(x, pltpu.HBM) for x in (
        conv_taps, document.reshape(1, -1), routes.T, route_weight.T, norm_gain.reshape(1, -1),
        outer_gate, inner_gate, values, mix_proj, stream, w_gate, w_up, w_down,
    )])


def solution(mesh):
    return jax.shard_map(
        body,
        mesh=mesh,
        in_specs=(
            P("sp", "tp"),
            P("sp", "tp"),
            P("sp", "tp"),
            P(None, "tp"),
            P("sp"),
            P("tp", None),
            P("sp", None),
            P(),
            P("sp", None),
            P("sp", None),
            P("sp", None, "tp"),
            P("sp", None, "tp"),
            P("sp", "tp", None),
        ),
        out_specs=P("sp", "tp"),
        check_vma=False,
    )
```

```python
import functools

import jax
import jax.numpy as jnp
from jax import lax
from jax.experimental import pallas as pl
from jax.experimental.pallas import tpu as pltpu
from jax.sharding import PartitionSpec as P

F32 = jnp.float32
BF16 = jnp.bfloat16
MESH = pl.DeviceIdType.MESH
HEAD = 16
TUNED = (
    (0, 0), (1, 0), (0, 1), (0, 2), (1, 1), (0, 4), (1, 2), (0, 3),
    (0, 5), (1, 4), (2, 0), (0, 6), (1, 5), (0, 7), (3, 0), (4, 0),
    (6, 0), (1, 6), (1, 3), (2, 2), (1, 7), (3, 2), (4, 2), (5, 5),
    (6, 2), (5, 4), (5, 0), (2, 3), (7, 5), (3, 3), (4, 3), (6, 3),
    (5, 6), (7, 4), (2, 1), (5, 7), (8, 5), (3, 1), (4, 1), (7, 6),
    (5, 3), (8, 4), (5, 2), (9, 5), (8, 6), (7, 7), (6, 1), (7, 3),
    (5, 1), (9, 4), (8, 7), (7, 2), (8, 3), (7, 1), (7, 0), (8, 2),
    (9, 3), (8, 1), (9, 6), (8, 0), (9, 0), (9, 7), (9, 1), (9, 2),
)


def general_plan(n_sp, group):
    plan, near = [], min(2, n_sp)

    def run(k, d, low=0):
        if low <= d < n_sp and (k, d) not in plan:
            plan.append((k, d))

    for k, d in ((0, 0), (0, 1), (1, 0), (1, 1), (0, 2), (0, 3), (1, 2)):
        run(k, d)
    for j in range(n_sp // group):
        first = j * group
        ahead, behind = range(first + 3, first + 3 + group), range(first - group, first)
        plan.append((2, j))
        for d in ahead:
            run(0, d + 1)
        plan.append((3, j))
        for d in ahead:
            run(1, d)
        plan.append((4, j))
        for d in range(first, first + group):
            run(5, d, near)
        plan.append((6, j))
        for d in behind:
            run(7, d, near)
        for d in behind:
            run(8, d - group, near)
        for d in behind:
            run(9, d - 3 * group, near)
    for d in range(near, n_sp):
        run(8, d - group, near)
        run(7, d, near)
        run(5, n_sp - 1 - d)
    for d in (1, 0):
        run(5, d)
    for d in range(near, n_sp):
        run(8, d)
    for d in (1, 0):
        run(7, d)
    for d in range(near, n_sp - 2):
        run(9, d)
    for d in (1, 0):
        run(8, d)
    for d in range(n_sp):
        run(9, d)
    return plan


def xor(value, mask, count):
    out, bit = value, 1
    while bit < count:
        if isinstance(mask, int):
            if mask & bit:
                out = out + bit * (1 - 2 * lax.rem(lax.div(value, bit), 2))
        else:
            ours = lax.rem(lax.div(value, bit), 2)
            other = lax.rem(lax.div(mask, bit), 2)
            out = out + bit * other * (1 - 2 * ours)
        bit *= 2
    return out


def kernel(
    n_sp, n_tp, cap,
    taps_hbm, doc_hbm, routes_hbm, rw_hbm, gain_hbm, outer_hbm, inner_hbm, vals_hbm, mix_hbm, stream_hbm, wg_hbm, wu_hbm, wd_hbm,
    out,
    taps, doc_r, routes_r, rw_r, gain, outer, inner, vals, own, wg, wu, wd, rim_out, rim_in, prod_pad, doc_pad,
    gbuf, mixb, hidden, obuf, xbuf, pbuf, r1, act, ret, back, acc,
    local_sem, rim_s, rim_r, ga_s, ga_r, mx_s, mx_r, z_s, z_r, ag_s, ag_r, rs_s, rs_r, bk_s, bk_r,
):
    s, p = lax.axis_index("sp"), lax.axis_index("tp")
    length, channels = outer.shape
    width = own.shape[1]
    features = mix_hbm.shape[1]
    hidden_units = wg.shape[1]
    x_side = 1
    while x_side * x_side < n_tp:
        x_side *= 2
    square = x_side * x_side == n_tp
    group = 2 if n_sp % 2 == 0 else 1
    firsts, seconds = range(x_side), range(n_tp // x_side)

    def at(index):
        return pl.multiple_of(index * width, width)

    masks = [m for m in (2, 1) if m < n_sp]
    pieces = 2 ** len(masks)
    piece = channels // pieces

    def piece_rows(mask):
        return pl.ds(pl.multiple_of(lax.rem(xor(s, mask, n_sp), pieces) * piece, piece), piece)

    loads = [
        pltpu.make_async_copy(inner_hbm, inner, local_sem.at[0]),
        pltpu.make_async_copy(vals_hbm, vals, local_sem.at[1]),
        pltpu.make_async_copy(outer_hbm, outer, local_sem.at[2]),
        pltpu.make_async_copy(mix_hbm.at[:, pl.ds(at(p), width)], mixb.at[0], local_sem.at[3]),
        pltpu.make_async_copy(stream_hbm.at[:, pl.ds(at(p), width)], own, local_sem.at[4]),
    ]
    weight_loads = [
        pltpu.make_async_copy(wg_hbm.at[0], wg, local_sem.at[5]),
        pltpu.make_async_copy(wu_hbm.at[0], wu, local_sem.at[6]),
        pltpu.make_async_copy(wd_hbm.at[0], wd, local_sem.at[7]),
    ]
    small_loads = [
        pltpu.make_async_copy(src, dst, local_sem.at[8 + k])
        for k, (src, dst) in enumerate(
            ((routes_hbm, routes_r), (rw_hbm, rw_r), (doc_hbm, doc_r), (taps_hbm, taps), (gain_hbm, gain))
        )
    ]
    for load in small_loads + loads:
        load.start()

    barrier = pltpu.get_barrier_semaphore()
    for d in range(1, n_sp):
        pl.semaphore_signal(barrier, inc=1, device_id={"sp": xor(s, d, n_sp)}, device_id_type=MESH)
    for r in range(1, n_tp):
        pl.semaphore_signal(barrier, inc=1, device_id={"tp": xor(p, r, n_tp)}, device_id_type=MESH)
    def send(src, dst, s_sem, r_sem, **device):
        pltpu.make_async_remote_copy(
            src_ref=src, dst_ref=dst, send_sem=s_sem, recv_sem=r_sem,
            device_id=device, device_id_type=MESH,
        ).start()

    def arrived(ref, sem):
        pltpu.make_async_copy(ref, ref, sem).wait()

    pl.semaphore_wait(barrier, n_sp - 1 + n_tp - 1)
    for r in range(n_tp - 1, 0, -1):
        peer = xor(p, r, n_tp)
        send(
            mix_hbm.at[piece_rows(0), pl.ds(at(peer), width)], mixb.at[r, piece_rows(0)],
            mx_s, mx_r.at[0, r], tp=peer,
        )

    def pass_on(r, mask, step):
        send(
            mixb.at[r, piece_rows(mask)], mixb.at[r, piece_rows(mask)],
            mx_s, mx_r.at[step, r], sp=xor(s, masks[-1] if step != 1 else masks[0], n_sp),
        )

    for load in small_loads:
        load.wait()
    lines = [routes_r[...].astype(F32), rw_r[...], doc_r[...].astype(F32)]
    table = jnp.concatenate(lines + [jnp.zeros((3, length), F32)], axis=0)
    table = jnp.concatenate([table] * 16, axis=0).T
    chosen = [table[:, 0:1], table[:, 1:2]]
    chosen_weight = [table[:, 2:3], table[:, 3:4]]
    docs = jnp.broadcast_to(table[:, 4:5], (length, channels))
    loads[0].wait()
    loads[1].wait()
    product = inner[...].astype(F32) * vals[...].astype(F32)
    prod_pad[8:, :] = product
    doc_pad[8:, :] = docs
    rim_out[:8, :] = product[length - 8 :]
    rim_out[8:, :] = docs[length - 8 :]
    kernel_taps = taps[...].astype(F32)

    def gated(count):
        conv = kernel_taps[2:3] * product[:count]
        for step in (1, 2):
            same = doc_pad[pl.ds(8 - step, count), :] == docs[:count]
            before = prod_pad[pl.ds(8 - step, count), :]
            conv = conv + kernel_taps[2 - step : 3 - step] * jnp.where(same, before, 0.0)
        return (outer[:count, :].astype(F32) * conv).astype(BF16)

    has_next = s < n_sp - 1
    rim = pltpu.make_async_remote_copy(
        src_ref=rim_out, dst_ref=rim_in, send_sem=rim_s, recv_sem=rim_r,
        device_id={"sp": lax.rem(s + 1, n_sp)}, device_id_type=MESH,
    )

    @pl.when(has_next)
    def _():
        rim.start()

    prod_pad[:8, :] = jnp.zeros((8, channels), F32)
    doc_pad[:8, :] = jnp.full((8, channels), -1.0, F32)
    loads[2].wait()
    gbuf[0] = gated(length)

    @pl.when(s > 0)
    def _():
        rim.wait_recv()
        prod_pad[:8, :] = rim_in[:8, :]
        doc_pad[:8, :] = rim_in[8:, :]
        gbuf[0, :HEAD] = gated(HEAD)

    for r in range(n_tp - 1, 0, -1):
        send(gbuf.at[0], gbuf.at[r], ga_s, ga_r.at[r], tp=xor(p, r, n_tp))
    for load in weight_loads:
        load.start()

    row = lax.broadcasted_iota(jnp.int32, (length, length), 0)
    col = lax.broadcasted_iota(jnp.int32, (length, length), 1)
    expert_r = lax.broadcasted_iota(jnp.int32, (max(n_sp, 16), length), 0)
    in_r = ((routes_r[0:1, :] == expert_r) | (routes_r[1:2, :] == expert_r)).astype(F32)
    rank_r = jnp.dot(in_r.astype(BF16), (row < col).astype(F32).astype(BF16), preferred_element_type=F32)
    expert_c = lax.broadcasted_iota(jnp.int32, (length, 128), 1).astype(F32)
    in_c = ((chosen[0] == expert_c) | (chosen[1] == expert_c)).astype(F32)
    rank_c = jnp.dot((row > col).astype(F32).astype(BF16), in_c.astype(BF16), preferred_element_type=F32)
    rank_r = jnp.where(in_r > 0, rank_r, -1.0)
    rank_c = jnp.where(in_c > 0, rank_c, -1.0)

    slot_r = lax.broadcasted_iota(jnp.int32, (cap, length), 0).astype(F32)
    turn = [0, 1, 3, 2, 5, 7, 4, 6] + list(range(8, n_sp))
    picks = []
    for d in range(n_sp):
        line = jnp.sum(jnp.where(expert_r == xor(s, turn[d], n_sp), rank_r, 0.0), axis=0, keepdims=True)
        picks.append((line == slot_r).astype(F32).astype(BF16))

    for r in range(n_tp - 1, 0, -1):
        arrived(mixb.at[r, piece_rows(0)], mx_r.at[0, r])
        if len(masks) == 2:
            pass_on(r, 0, 1)
        if masks:
            pass_on(r, 0, 2)
    loads[3].wait()
    loads[4].wait()
    total = own[...].astype(F32) + jnp.dot(gbuf[0], mixb[0], preferred_element_type=F32)
    if len(masks) == 2:
        for r in range(n_tp - 1, 0, -1):
            arrived(mixb.at[r, piece_rows(2)], mx_r.at[1, r])
            pass_on(r, 2, 3)
    for r in range(n_tp - 1, 0, -1):
        if masks:
            arrived(mixb.at[r, piece_rows(1)], mx_r.at[2, r])
        if len(masks) == 2:
            arrived(mixb.at[r, piece_rows(3)], mx_r.at[3, r])
        arrived(gbuf.at[r], ga_r.at[r])
        total = total + jnp.dot(gbuf[r], mixb[r], preferred_element_type=F32)
    hidden[...] = total
    scaled = (total * gain[:, pl.ds(at(p), width)]).astype(BF16)

    for d in range(n_sp):
        rows = jnp.dot(picks[d], scaled, preferred_element_type=F32).astype(BF16)
        if d == 0:
            xbuf[0, 0] = rows
        else:
            obuf[d] = rows
            send(obuf.at[d], xbuf.at[0, d], z_s, z_r.at[d], sp=xor(s, turn[d], n_sp))

    def axes(d):
        side = lax.rem(s + d // group, 2) * (x_side - 1) if square else 0
        return 1 + side, x_side - side

    def gather_first(d):
        u, _ = axes(d)
        if d:
            arrived(xbuf.at[0, d], z_r.at[d])
        for k in firsts[1:]:
            f = k * u
            send(xbuf.at[0, d], xbuf.at[f, d], ag_s, ag_r.at[d, f], tp=xor(p, f, n_tp))

    def gather_second(d):
        u, v = axes(d)
        for k in firsts:
            f = k * u
            if k:
                arrived(xbuf.at[f, d], ag_r.at[d, f])
            for l in seconds[1:]:
                g = l * v
                send(
                    xbuf.at[f, d], xbuf.at[f + g, d], ag_s, ag_r.at[d, f + g],
                    tp=xor(p, g, n_tp),
                )

    tile = min(256, hidden_units)
    tiles = hidden_units // tile

    scales = {}

    def members(j):
        return slice(j * group, (j + 1) * group)

    def up_part(j, low, high):
        def up_tile(i, _):
            lanes = pl.ds(pl.multiple_of(i * tile, tile), tile)
            gate = jnp.zeros((group * cap, tile), F32)
            upper = jnp.zeros((group * cap, tile), F32)
            for r in range(n_tp):
                lhs = xbuf[r, members(j)].reshape(group * cap, width)
                deep = pl.ds(at(xor(p, r, n_tp)), width)
                gate = gate + jnp.dot(lhs, wg[deep, lanes], preferred_element_type=F32)
                upper = upper + jnp.dot(lhs, wu[deep, lanes], preferred_element_type=F32)
            gate, upper = gate * scales[j], upper * scales[j]
            act[:, lanes] = (gate / (1.0 + jnp.exp(-gate)) * upper).astype(BF16)
            return 0

        lax.fori_loop(low, high, up_tile, 0)

    def up_first(j):
        if not scales:
            for load in weight_loads:
                load.wait()
        u, v = axes(j * group)
        for d in range(j * group, (j + 1) * group):
            for k in firsts:
                for l in seconds[1:]:
                    arrived(xbuf.at[k * u + l * v, d], ag_r.at[d, k * u + l * v])
        power = jnp.zeros((group * cap, 1), F32)
        for r in range(n_tp):
            inverse = 1.0 / gain[:, pl.ds(at(xor(p, r, n_tp)), width)]
            plain = xbuf[r, members(j)].reshape(group * cap, width).astype(F32) * inverse
            power = power + jnp.sum(plain * plain, axis=1, keepdims=True)
        scales[j] = lax.rsqrt(power / features + 1e-06)
        up_part(j, 0, tiles // 2)

    def up_second(j):
        up_part(j, tiles // 2, tiles)

    def down_part(j, low, high):
        u, v = axes(j * group)
        for k in range(low, high):
            for l in seconds[::-1]:
                r = k * u + l * v
                lanes = pl.ds(at(xor(p, r, n_tp)), width)
                part = jnp.dot(act[...], wd[:, lanes], preferred_element_type=F32).astype(BF16)
                pbuf[r, members(j)] = part.reshape(group, cap, width)

    def down_first(j):
        down_part(j, 1, len(firsts))

    def down_second(j):
        down_part(j, 0, 1)

    def scatter_first(d):
        u, v = axes(d)
        for k in firsts[:0:-1]:
            for l in seconds[::-1]:
                r = k * u + l * v
                send(pbuf.at[r, d], r1.at[r, d], rs_s, rs_r.at[d, r], tp=xor(p, k * u, n_tp))

    def scatter_second(d):
        u, v = axes(d)
        for l in seconds[1:]:
            g = l * v
            part = pbuf[g, d].astype(F32)
            for k in firsts[1:]:
                arrived(r1.at[k * u + g, d], rs_r.at[d, k * u + g])
                part = part + r1[k * u + g, d].astype(F32)
            pbuf[g, d] = part.astype(BF16)
            send(pbuf.at[g, d], r1.at[g, d], rs_s, rs_r.at[d, g], tp=xor(p, g, n_tp))

    def give_back(d):
        u, v = axes(d)
        part = pbuf[0, d].astype(F32)
        for k in [k * u for k in firsts[1:]] + [l * v for l in seconds[1:]]:
            arrived(r1.at[k, d], rs_r.at[d, k])
            part = part + r1[k, d].astype(F32)
        if d == 0:
            back[0] = part.astype(BF16)
        else:
            ret[d] = part.astype(BF16)
            send(ret.at[d], back.at[d], bk_s, bk_r.at[d], sp=xor(s, turn[d], n_sp))

    slot_c = lax.broadcasted_iota(jnp.int32, (length, cap), 1).astype(F32)
    acc[...] = hidden[...]

    def combine(d):
        e = xor(s, turn[d], n_sp)
        if d:
            arrived(back.at[d], bk_r.at[d])
        line = jnp.sum(jnp.where(expert_c == e.astype(F32), rank_c, 0.0), axis=1, keepdims=True)
        pick = (line == slot_c).astype(F32).astype(BF16)
        fetched = jnp.dot(pick, back[d], preferred_element_type=F32)
        weight = sum(jnp.where(c == e.astype(F32), w, 0.0) for c, w in zip(chosen, chosen_weight))
        acc[...] = acc[...] + fetched * weight

    stages = (
        gather_first, gather_second, up_first, up_second, down_first,
        scatter_first, down_second, scatter_second, give_back, combine,
    )
    plan = general_plan(n_sp, group)
    plan = TUNED if len(TUNED) == len(plan) else plan
    for k, d in plan[:-1]:
        stages[k](d)
    arrived(xbuf.at[0, pl.ds(1, n_sp - 1)], z_s)
    arrived(back.at[pl.ds(1, n_sp - 1)], bk_s)
    arrived(gbuf.at[pl.ds(1, n_tp - 1)], ga_s)
    arrived(xbuf.at[pl.ds(1, n_tp - 1)], ag_s)
    arrived(r1.at[pl.ds(1, n_tp - 1)], rs_s)
    arrived(mixb.at[pl.ds(1, n_tp - 1)], mx_s)
    stages[plan[-1][0]](plan[-1][1])
    out[...] = acc[...].astype(out.dtype)
    @pl.when(has_next)
    def _():
        rim.wait_send()


def body(
    outer_gate, inner_gate, values, conv_taps, document, mix_proj, stream, norm_gain,
    routes, route_weight, w_gate, w_up, w_down,
):
    length, features = stream.shape
    channels = outer_gate.shape[1]
    n_sp, n_tp = lax.axis_size("sp"), lax.axis_size("tp")
    width = features // n_tp
    units = w_gate.shape[2]
    cap = -(-(3 * length // n_sp) // 16) * 16
    vmem, hbm = pl.BlockSpec(memory_space=pltpu.VMEM), pl.BlockSpec(memory_space=pltpu.HBM)
    block = (n_sp, cap, width)
    dma = pltpu.SemaphoreType.DMA
    return pl.pallas_call(
        functools.partial(kernel, n_sp, n_tp, cap),
        out_shape=pltpu.VMEM((length, width), BF16),
        in_specs=[hbm] * 13,
        out_specs=vmem,
        scratch_shapes=[
            pltpu.VMEM(conv_taps.shape, BF16),
            pltpu.VMEM((1, length), jnp.int32),
            pltpu.VMEM((2, length), jnp.int32),
            pltpu.VMEM((2, length), F32),
            pltpu.VMEM((1, features), F32),
            pltpu.VMEM((length, channels), BF16),
            pltpu.VMEM((length, channels), BF16),
            pltpu.VMEM((length, channels), BF16),
            pltpu.VMEM((length, width), BF16),
            pltpu.VMEM((features, units), BF16),
            pltpu.VMEM((features, units), BF16),
            pltpu.VMEM((units, features), BF16),
            pltpu.VMEM((16, channels), F32),
            pltpu.VMEM((16, channels), F32),
            pltpu.VMEM((length + 8, channels), F32),
            pltpu.VMEM((length + 8, channels), F32),
            pltpu.VMEM((n_tp, length, channels), BF16),
            pltpu.VMEM((n_tp, channels, width), BF16),
            pltpu.VMEM((length, width), F32),
            pltpu.VMEM(block, BF16),
            pltpu.VMEM((n_tp,) + block, BF16),
            pltpu.VMEM((n_tp,) + block, BF16),
            pltpu.VMEM((n_tp,) + block, BF16),
            pltpu.VMEM(((2 if n_sp % 2 == 0 else 1) * cap, units), BF16),
            pltpu.VMEM(block, BF16),
            pltpu.VMEM(block, BF16),
            pltpu.VMEM((length, width), F32),
            dma((13,)), dma, dma, dma, dma((n_tp,)), dma, dma((4, n_tp)), dma, dma((n_sp,)),
            dma, dma((n_sp, n_tp)), dma, dma((n_sp, n_tp)),
            dma, dma((n_sp,)),
        ],
        compiler_params=pltpu.CompilerParams(
            collective_id=0, has_side_effects=True, vmem_limit_bytes=40 << 20
        ),
    )(*[pltpu.with_memory_space_constraint(x, pltpu.HBM) for x in (
        conv_taps, document.reshape(1, -1), routes.T, route_weight.T, norm_gain.reshape(1, -1),
        outer_gate, inner_gate, values, mix_proj, stream, w_gate, w_up, w_down,
    )])


def solution(mesh):
    return jax.shard_map(
        body,
        mesh=mesh,
        in_specs=(
            P("sp", "tp"),
            P("sp", "tp"),
            P("sp", "tp"),
            P(None, "tp"),
            P("sp"),
            P("tp", None),
            P("sp", None),
            P(),
            P("sp", None),
            P("sp", None),
            P("sp", None, "tp"),
            P("sp", None, "tp"),
            P("sp", "tp", None),
        ),
        out_specs=P("sp", "tp"),
        check_vma=False,
    )
```
